32 devices in a mesh: ep: 8 (over z, core), tp: 4 (over y, x).
Axes of the slice: x: 2, y: 2, z: 4, core: 2. Of those that a mesh axis runs over, the one named last changes fastest.
Arguments:
- tokens: bfloat16 [256, 2560], P('ep'), may hold values from -6 to 6
- norm_gain: float32 [2560], replicated, may hold values from 0.1 to 1.9
- route: int32 [256, 4], P('ep'), may hold values from 0 to 7, all different within a row; in each aligned block of 32 rows (0 to 31, 32 to 63, ...) at most 24 rows name the same one
- route_weight: float32 [256, 4], P('ep'), may hold values from 0.1 to 1
- gate_weight: bfloat16 [8, 8960, 2560], P('ep', 'tp'), may hold values from -0.125 to 0.125
- up_weight: bfloat16 [8, 8960, 2560], P('ep', 'tp'), may hold values from -0.125 to 0.125
- down_weight: bfloat16 [8, 8960, 2560], P('ep', 'tp'), may hold values from -0.0625 to 0.0625
Outputs:
- mixed: bfloat16 [256, 2560], P('ep', 'tp')
The draws below stay inside these ranges and needn't reach their ends.
Inputs may be any that keep to these rules, and one draw needn't show every extreme that they name: `route`: each row names 4 different experts. Among the rows of one index of ep no expert is named more than 24 times, a bound that some block reaches.
All inputs are finite; a program needn't handle non-finite values.
Results may differ from the reference program's by a relative error of at most 0.018.
Values may be sent and summed in bfloat16 or wider, within the bound.
A program may use at most 128 MiB of HBM per device.

```python
import math
import jax
import jax.numpy as jnp
import numpy as np
from jax import lax

D = 2560
FF = 8960
TOP_K = 4
TOK_DEV = 32
EXPERTS = 8
TOKENS = 256
CAP = 24
N_EP = 8
N_TP = 4


def block_levels(own_key, dims, shards, least, top_value):
    loudness = 1.0
    for axis_at, blocks in shards:
        steps = jax.random.uniform(jax.random.fold_in(jax.random.fold_in(own_key, 6), axis_at), (blocks,), jnp.float32, least / len(shards), top_value / len(shards))
        loudness = loudness * jnp.repeat(jnp.exp(steps), dims[axis_at] // blocks).reshape((-1,) + (1,) * (len(dims) - 1 - axis_at))
    return loudness


def shared_out(own_key, own, number, rows, number_of, top, limit, lean):
    ranking = jax.random.permutation(own_key, number_of)
    packed, common = shares(number_of, rows * top, limit, lean, True), shares(number_of, rows * top, limit, lean, False)
    places = jnp.arange(number_of)

    def named(tallies, rotation):
        used = int((tallies > 0).sum())
        fixed = max(1, used // 4)
        shifted = fixed + (places - fixed + rotation * (used - fixed)) % max(1, number_of - fixed)
        return jnp.zeros((number_of,), jnp.int32).at[ranking[jnp.where(places < fixed, places, shifted)]].set(jnp.asarray(tallies, jnp.int32))

    tallies = jnp.where(number % 4 == 0, named(packed, number // 4), named(common, number - number // 4 - 1))
    mixed = jax.random.permutation(jax.random.fold_in(own, 3), number_of)
    donor, taker = mixed[0:number_of // 2 * 2:2], mixed[1:number_of // 2 * 2:2]
    room = jnp.minimum(tallies[donor] - 1, limit - tallies[taker]) // 2
    room = jnp.where((donor == ranking[0]) | (taker == ranking[0]) | (tallies[taker] == 0), 0, jnp.maximum(room, 0))
    shifted = jax.random.randint(jax.random.fold_in(own, 4), (number_of // 2,), 0, 1 << 20) % (room + 1)
    tallies = tallies.at[donor].add(-shifted).at[taker].add(shifted)
    labels = jnp.searchsorted(jnp.cumsum(tallies), jnp.arange(rows * top), side="right").astype(jnp.int32)
    listing = labels.reshape(top, rows).T
    listing = listing[jax.random.permutation(jax.random.fold_in(own, 1), rows)]
    rotation = jax.random.randint(jax.random.fold_in(own, 2), (rows, 1), 0, top)
    return jnp.take_along_axis(listing, (jnp.arange(top)[None, :] + rotation) % top, axis=1)


def shares(number_of, total, most, slope, full):
    loads = [(1 << 20) // math.isqrt(standing ** slope) + 1 for standing in range(1, number_of + 1)]
    largest = most if full else min(most, max(-(-total // number_of), total * loads[0] // sum(loads)))
    least = 1 if total - largest >= number_of - 1 else 0
    counts, rest = [largest] + [least] * (number_of - 1), total - largest - least * (number_of - 1)
    while rest > 0:
        movable = [i for i in range(1, number_of) if counts[i] < largest] or [i for i in range(1, number_of) if counts[i] < most]
        whole, remaining = sum([loads[i] for i in movable]), rest
        for i in movable:
            addition = min(most - counts[i], max(1, remaining * loads[i] // whole), rest)
            counts[i] = counts[i] + addition
            rest = rest - addition
    return np.array(counts)


def normal_values(stream_key, dims, spread, bound, cuts=(), kind=jnp.bfloat16):
    entries = jax.random.normal(stream_key, dims, jnp.float32) * spread
    if len(cuts) > 0:
        entries = block_levels(stream_key, dims, cuts, -0.22, 0.18) * entries
    return jnp.clip(entries, min=-bound, max=bound).astype(kind)


def setup_inputs(seed: int = 0) -> dict:
    streams_of = jax.random.split(jax.random.key(seed), 8)
    tokens = normal_values(streams_of[0], (TOKENS, D), 1.0, 6.0, ((0, 8),))
    norm_gain = jnp.clip(1.0 + 0.18 * jax.random.normal(streams_of[1], (D,), jnp.float32), 0.1, 1.9)
    route_keys = jax.random.split(jax.random.fold_in(streams_of[2], 1), TOKENS // TOK_DEV)
    route_turns = jax.random.permutation(jax.random.fold_in(streams_of[2], 3), TOKENS // TOK_DEV)
    route = jax.vmap(lambda own, number: shared_out(jax.random.fold_in(streams_of[2], 2), own, number, TOK_DEV, EXPERTS, TOP_K, CAP, 2))(route_keys, route_turns).reshape((TOKENS, TOP_K))
    route_weight = jnp.clip(0.1 + 0.9 * jax.random.uniform(streams_of[3], (TOKENS, TOP_K), jnp.float32) ** block_levels(streams_of[3], (TOKENS, TOP_K), ((0, 8),), -0.2, 0.2), 0.1, 1.0)
    gate_weight = normal_values(streams_of[4], (EXPERTS, FF, D), D ** -0.5, 0.125, ((0, 8), (1, 4)))
    up_weight = normal_values(streams_of[5], (EXPERTS, FF, D), D ** -0.5, 0.125, ((0, 8), (1, 4)))
    down_weight = normal_values(streams_of[6], (EXPERTS, FF, D), FF ** -0.5, 0.0625, ((0, 8), (1, 4)))
    return {"tokens": tokens, "norm_gain": norm_gain, "route": route, "route_weight": route_weight, "gate_weight": gate_weight, "up_weight": up_weight, "down_weight": down_weight}


epsilon = 1e-06

def reference(tokens, norm_gain, route, route_weight, gate_weight, up_weight, down_weight):
    values = tokens.astype(jnp.float32)
    scaled = values * lax.rsqrt(lax.optimization_barrier(jnp.mean(values * values, axis=-1, keepdims=True)) + epsilon)
    normed = (scaled * norm_gain).astype(jnp.bfloat16)
    flat_route = route.reshape(N_EP, TOK_DEV * TOP_K)
    onehot = (flat_route[:, :, None] == jnp.arange(EXPERTS, dtype=jnp.int32)[None, None, :]).astype(jnp.int32)
    slot_number = lax.optimization_barrier(jnp.sum((jnp.cumsum(onehot, axis=1) - 1) * onehot, axis=-1)).astype(jnp.int32)
    source = jnp.arange(N_EP, dtype=jnp.int32)[:, None]
    slot_index = ((flat_route * N_EP + source) * CAP + slot_number).reshape(TOKENS * TOP_K).astype(jnp.int32)
    repeated = jnp.repeat(normed, TOP_K, axis=0)
    buffer = jnp.zeros((EXPERTS * N_EP * CAP, D), jnp.bfloat16).at[slot_index].set(repeated)
    buffer = buffer.reshape(EXPERTS, N_EP * CAP, D)

    def expert(operands):
        inputs, w_gate, w_up, w_down = operands
        gate = jnp.dot(inputs, w_gate.T, preferred_element_type=jnp.float32)
        upward = jnp.dot(inputs, w_up.T, preferred_element_type=jnp.float32)
        hidden = (jax.nn.silu(gate) * upward).astype(jnp.bfloat16)
        hidden_blocks = hidden.reshape(N_EP * CAP, N_TP, FF // N_TP).astype(jnp.float32)
        down_blocks = w_down.reshape(N_TP, FF // N_TP, D).astype(jnp.float32)
        block_sum = jnp.einsum('rbf,bfd->brd', hidden_blocks, down_blocks).astype(jnp.bfloat16)
        block_sum = lax.optimization_barrier(block_sum)
        return lax.optimization_barrier(jnp.sum(block_sum.astype(jnp.float32), axis=0)).astype(jnp.bfloat16)
    results = lax.map(expert, (buffer, gate_weight, up_weight, down_weight)).reshape(EXPERTS * N_EP * CAP, D)
    picked = results[slot_index].reshape(TOKENS, TOP_K, D).astype(jnp.float32)
    mixed = lax.optimization_barrier(jnp.sum(route_weight[:, :, None] * picked, axis=1))
    return mixed.astype(jnp.bfloat16)
```

```python
import functools

import jax
import jax.numpy as jnp
from jax import lax
from jax.experimental import pallas as pl
from jax.experimental.pallas import tpu as pltpu
from jax.sharding import PartitionSpec as P

epsilon = 1e-06


def on_device(tokens, norm_gain, route, route_weight, gate_weight, up_weight, down_weight):
    tok_rows, width = tokens.shape
    top_count = route.shape[1]
    local_experts = gate_weight.shape[0]
    ep_count = lax.axis_size("ep")
    tp_count = lax.axis_size("tp")
    experts = local_experts * ep_count
    capacity = min(tok_rows, max(2, (3 * tok_rows * top_count + 2 * experts - 1) // (2 * experts)))
    width_share = width // tp_count
    values = tokens.astype(jnp.float32)
    scaled = values * lax.rsqrt(jnp.mean(values * values, axis=-1, keepdims=True) + epsilon)
    normed = (scaled * norm_gain).astype(jnp.bfloat16)
    flat_route = route.reshape(tok_rows * top_count)
    onehot = (flat_route[:, None] == jnp.arange(experts, dtype=jnp.int32)[None, :]).astype(
        jnp.int32
    )
    slot_number = jnp.sum((jnp.cumsum(onehot, axis=0) - 1) * onehot, axis=-1)
    slot_index = flat_route * capacity + slot_number
    placing = (
        slot_index[None, :] == jnp.arange(experts * capacity, dtype=jnp.int32)[:, None]
    ).astype(jnp.bfloat16)
    repeated = jnp.repeat(normed, top_count, axis=0)
    columns = lax.dynamic_slice_in_dim(repeated, lax.axis_index("tp") * width_share, width_share, 1)
    send = jnp.dot(placing, columns, preferred_element_type=jnp.float32).astype(jnp.bfloat16)
    send = send.reshape(ep_count, local_experts, capacity, width_share)
    arrived = lax.all_to_all(send, "ep", split_axis=0, concat_axis=0, tiled=True)
    piece = lax.all_gather(arrived, "tp", axis=3, tiled=True)
    gate = jnp.einsum("sjcd,jfd->sjcf", piece, gate_weight, preferred_element_type=jnp.float32)
    upward = jnp.einsum("sjcd,jfd->sjcf", piece, up_weight, preferred_element_type=jnp.float32)
    hidden = (jax.nn.silu(gate) * upward).astype(jnp.bfloat16)
    partial_value = jnp.einsum(
        "sjcf,jfd->sjcd", hidden, down_weight, preferred_element_type=jnp.float32
    )
    shares = lax.psum_scatter(
        partial_value.astype(jnp.bfloat16), "tp", scatter_dimension=3, tiled=True
    )
    returned = lax.all_to_all(shares, "ep", split_axis=0, concat_axis=0, tiled=True)
    results = returned.reshape(experts * capacity, width_share)
    picked = results[slot_index].reshape(tok_rows, top_count, width_share).astype(jnp.float32)
    mixed = jnp.sum(route_weight[:, :, None] * picked, axis=1)
    return mixed.astype(jnp.bfloat16)

MESH = pl.DeviceIdType.MESH
CORES = 2
F32 = jnp.float32
BF16 = jnp.bfloat16
NT = (((1,), (1,)), ((), ()))


def row_blocks(total, size):
    return [(at, min(size, total - at)) for at in range(0, total, size)]


def fused(
    nz, side, tokens_ref, gain_ref, route_ref, weight_ref, gate_hbm, up_hbm, down_hbm, out_ref,
    wg, wu, wd, xg, acc_g, acc_u, hid, ob, sib, ss, rp, zs, zr, wsend, wrecv,
    w_sem, z_ssem, z_rsem, own_ssem, own_rsem, f_ssem, f_rsem, t_ssem, t_rsem,
    r_ssem, r_rsem, s_ssem, s_rsem, x_ssem, x_rsem, y_ssem, y_rsem,
):
    ep, tp = lax.axis_index("ep"), lax.axis_index("tp")
    n_tp, n_ep = side * side, nz * CORES
    z, core = ep // CORES, ep % CORES
    ty, tx = tp // side, tp % side
    rows, width = tokens_ref.shape
    share = width // n_tp
    half = nz * rows

    def z_at(dz):
        return lax.rem(z + dz, nz)

    def from_z(dz):
        return lax.rem(z + nz - dz, nz)

    def quarter(r):
        return lax.rem(ty + r // side, side) * side + lax.rem(tx + r % side, side)

    def ep_id(zz, cc):
        return zz * CORES + cc

    other = 1 - core
    sibling = ep_id(z, other)

    def part(r):
        return pl.ds(r * share, share)

    def place(cc, zz):
        return pl.ds(pl.multiple_of((cc * nz + zz) * rows, rows), rows)

    loads = {}
    for r in range(n_tp):
        cols = pl.ds(pl.multiple_of(quarter(r) * share, share), share)
        for which, (hbm, vmem) in enumerate(((gate_hbm, wg), (up_hbm, wu), (down_hbm, wd))):
            loads[which, r] = pltpu.make_async_copy(
                hbm.at[0, :, cols], vmem.at[:, part(r)], w_sem.at[which, r]
            )
    for r in range(n_tp):
        loads[0, r].start()
        loads[1, r].start()
    for r in reversed(range(n_tp)):
        loads[2, r].start()

    barrier = pltpu.get_barrier_semaphore()
    for step in range(1, n_ep):
        pl.semaphore_signal(
            barrier, inc=1, device_id={"ep": lax.rem(ep + step, n_ep)}, device_id_type=MESH
        )
    for r in range(1, n_tp):
        pl.semaphore_signal(barrier, inc=1, device_id={"tp": quarter(r)}, device_id_type=MESH)

    values = tokens_ref[...].astype(F32)
    scaled = values * lax.rsqrt(jnp.mean(values * values, axis=-1, keepdims=True) + epsilon)
    normed = (scaled * gain_ref[...]).astype(BF16)
    for q in range(n_tp):
        qy, qx = q // side, q % side
        rel = lax.rem(qy + side - ty, side) * side + lax.rem(qx + side - tx, side)
        xg[place(core, z), pl.ds(pl.multiple_of(rel * share, share), share)] = normed[
            :, q * share : (q + 1) * share
        ]
    position = (core * nz + z) * rows
    lanes = lax.broadcasted_iota(jnp.int32, (rows, n_ep * rows), 1)
    sublanes = lax.broadcasted_iota(jnp.int32, (rows, n_ep * rows), 0)
    spread = lanes == sublanes + position
    route, route_weight = route_ref[...], weight_ref[...]
    for e in range(n_ep):
        chosen = jnp.sum(jnp.where(route == e, route_weight, 0.0), axis=1, keepdims=True)
        wsend[e] = jnp.sum(jnp.where(spread, chosen, 0.0), axis=0, keepdims=True)
    pl.semaphore_wait(barrier, n_ep + n_tp - 2)

    def remote(src, dst, ssem, rsem, target):
        return pltpu.make_async_remote_copy(
            src_ref=src, dst_ref=dst, send_sem=ssem, recv_sem=rsem,
            device_id=target, device_id_type=MESH,
        )

    sent = []

    def go(copy):
        copy.start()
        sent.append(copy)
        return copy

    z_order = [dz for d in range(1, nz) for dz in ((d, nz - d) if d < nz - d else (d,)) if d <= nz - d]
    z_copy = {}
    own = (place(core, z), part(0))
    for dz in z_order:
        z_copy[dz] = go(remote(
            xg.at[own], xg.at[own], z_ssem.at[dz], z_rsem.at[dz], {"ep": ep_id(z_at(dz), core)}
        ))
    own_copy = go(remote(
        xg.at[place(core, z)], xg.at[place(core, z)], own_ssem, own_rsem, {"ep": sibling}
    ))
    w_copy = []
    for step in range(1, n_ep):
        to = lax.rem(ep + step, n_ep)
        w_copy.append(go(remote(
            wsend.at[to], wrecv.at[step], r_ssem.at[step], r_rsem.at[step], {"ep": to}
        )))

    forward, t_copy = {}, {}
    for dz in z_order:
        z_copy[dz].wait_recv()
        block = (place(core, from_z(dz)), part(0))
        forward[0, dz] = go(remote(
            xg.at[block], xg.at[block], f_ssem.at[0, dz], f_rsem.at[0, dz], {"ep": sibling}
        ))
        for r in range(1, n_tp - 1):
            there = (place(core, from_z(dz)), part(r))
            t_copy[r, dz] = go(remote(
                xg.at[block], xg.at[there], t_ssem.at[r, dz], t_rsem.at[r, dz], {"tp": quarter(r)}
            ))
    for dz in z_order:
        r = n_tp - 1
        block, there = (place(core, from_z(dz)), part(0)), (place(core, from_z(dz)), part(r))
        t_copy[r, dz] = go(remote(
            xg.at[block], xg.at[there], t_ssem.at[r, dz], t_rsem.at[r, dz], {"tp": quarter(r)}
        ))

    def pass_on(r):
        for dz in z_order:
            t_copy[r, dz].wait_recv()
            block = (place(core, from_z(dz)), part(r))
            forward[r, dz] = go(remote(
                xg.at[block], xg.at[block], f_ssem.at[r, dz], f_rsem.at[r, dz], {"ep": sibling}
            ))

    def forwarded(r):
        for dz in z_order:
            forward[r, dz].wait_recv()

    hidden_rows = wg.shape[0]
    blocks = row_blocks(hidden_rows, 5 * 128)
    own_copy.wait_recv()
    forwarded(0)

    def project(first, last):
        cols = slice(first * share, last * share)
        for r in range(first, last):
            loads[0, r].wait()
            loads[1, r].wait()
        held = xg[:, cols]
        for at, size in blocks:
            for weights, acc in ((wg, acc_g), (wu, acc_u)):
                term = lax.dot_general(
                    weights[at : at + size, cols], held, NT, preferred_element_type=F32
                )
                acc[at : at + size, :] = term if first == 0 else acc[at : at + size, :] + term

    project(0, 1)
    for r in range(1, n_tp - 1):
        pass_on(r)
    for r in range(1, n_tp - 1):
        forwarded(r)
    project(1, n_tp - 1)
    pass_on(n_tp - 1)
    forwarded(n_tp - 1)
    for copy in w_copy:
        copy.wait_recv()
    mix = wsend[ep]
    for step in range(1, n_ep):
        mix = mix + wrecv[step]
    last = n_tp - 1
    loads[0, last].wait()
    loads[1, last].wait()
    cols = slice(last * share, n_tp * share)
    held = xg[:, cols]
    for at, size in blocks:
        gate = acc_g[at : at + size, :] + lax.dot_general(
            wg[at : at + size, cols], held, NT, preferred_element_type=F32
        )
        upward = acc_u[at : at + size, :] + lax.dot_general(
            wu[at : at + size, cols], held, NT, preferred_element_type=F32
        )
        mixed_hidden = (gate / (1.0 + jnp.exp(-gate))) * upward * mix
        hid[:, at : at + size] = mixed_hidden.T.astype(BF16)

    mine = pl.ds(pl.multiple_of(core * half, half), half)
    yours = pl.ds(pl.multiple_of(other * half, half), half)
    back_order = list(reversed(range(n_tp)))
    far_order = list(reversed(z_order))
    s_copy, x_copy = {}, {}

    def combine(r):
        s_copy[r].wait_recv()
        total = ob[r, mine, :].astype(F32) + sib[r].astype(F32)
        ss[r] = total.astype(BF16)
        if r > 0:
            for dz in far_order + [0]:
                block = pl.ds(pl.multiple_of(z_at(dz) * rows, rows), rows)
                x_copy[r, dz] = go(remote(
                    ss.at[r, block, :], rp.at[r, block, :], x_ssem.at[r, dz], x_rsem.at[r, dz],
                    {"tp": quarter(r)},
                ))

    for k, r in enumerate(back_order):
        loads[2, r].wait()
        product = jnp.dot(hid[...], wd[:, r * share : (r + 1) * share], preferred_element_type=F32)
        ob[r] = product.astype(BF16)
        s_copy[r] = go(remote(
            ob.at[r, yours, :], sib.at[r], s_ssem.at[r], s_rsem.at[r], {"ep": sibling}
        ))
        if k > 0:
            combine(back_order[k - 1])
    combine(0)
    y_copy = {}
    for dz in far_order + [0]:
        block = pl.ds(pl.multiple_of(z_at(dz) * rows, rows), rows)
        total = ss[0, block, :].astype(F32)
        for r in range(1, n_tp):
            x_copy[r, dz].wait_recv()
            total = total + rp[r, block, :].astype(F32)
        if dz > 0:
            zs[dz] = total.astype(BF16)
            y_copy[dz] = go(remote(
                zs.at[dz], zr.at[dz], y_ssem.at[dz], y_rsem.at[dz], {"ep": ep_id(z_at(dz), core)}
            ))
    for dz in far_order:
        y_copy[dz].wait_recv()
        total = total + zr[dz].astype(F32)
    out_ref[...] = total.astype(BF16)
    for copy in sent:
        copy.wait_send()


def fused_call(nz, side, tokens, norm_gain, route, route_weight, gate_weight, up_weight, down_weight):
    rows, width = tokens.shape
    n_tp, n_ep = side * side, nz * CORES
    share, every, half = width // n_tp, n_ep * rows, nz * rows
    hidden = gate_weight.shape[1]
    vmem, dma = pltpu.VMEM, pltpu.SemaphoreType.DMA
    return pl.pallas_call(
        functools.partial(fused, nz, side),
        out_shape=jax.ShapeDtypeStruct((rows, share), BF16),
        in_specs=[pl.BlockSpec(memory_space=pltpu.VMEM)] * 4
        + [pl.BlockSpec(memory_space=pl.ANY)] * 3,
        out_specs=pl.BlockSpec(memory_space=pltpu.VMEM),
        scratch_shapes=[
            vmem((hidden, width), BF16),
            vmem((hidden, width), BF16),
            vmem((hidden, width), BF16),
            vmem((every, width), BF16),
            vmem((hidden, every), F32),
            vmem((hidden, every), F32),
            vmem((every, hidden), BF16),
            vmem((n_tp, every, share), BF16),
            vmem((n_tp, half, share), BF16),
            vmem((n_tp, half, share), BF16),
            vmem((n_tp, half, share), BF16),
            vmem((nz, rows, share), BF16),
            vmem((nz, rows, share), BF16),
            vmem((n_ep, 1, every), F32),
            vmem((n_ep, 1, every), F32),
            dma((3, n_tp)),
            dma((nz,)), dma((nz,)),
            dma, dma,
            dma((n_tp, nz)), dma((n_tp, nz)),
            dma((n_tp, nz)), dma((n_tp, nz)),
            dma((n_ep,)), dma((n_ep,)),
            dma((n_tp,)), dma((n_tp,)),
            dma((n_tp, nz)), dma((n_tp, nz)),
            dma((nz,)), dma((nz,)),
        ],
        compiler_params=pltpu.CompilerParams(
            collective_id=0, has_side_effects=True, vmem_limit_bytes=60 * 1024 * 1024
        ),
    )(tokens, norm_gain[None, :], route, route_weight, gate_weight, up_weight, down_weight)


def solution(mesh):
    n_ep, n_tp = mesh.shape["ep"], mesh.shape["tp"]
    side = 2

    def body(tokens, norm_gain, route, route_weight, gate_weight, up_weight, down_weight):
        args = (tokens, norm_gain, route, route_weight, gate_weight, up_weight, down_weight)
        fits = (
            n_tp == side * side
            and n_ep % CORES == 0
            and gate_weight.shape[0] == 1
            and tokens.shape[0] % 16 == 0
            and tokens.shape[1] % (128 * n_tp) == 0
            and gate_weight.shape[1] % 16 == 0
        )
        if fits:
            return fused_call(n_ep // CORES, side, *args)
        return on_device(*args)

    placed = (
        P("ep", None),
        P(),
        P("ep", None),
        P("ep", None),
        P("ep", "tp", None),
        P("ep", "tp", None),
        P("ep", "tp", None),
    )
    return jax.shard_map(
        body, mesh=mesh, in_specs=placed, out_specs=P("ep", "tp"), check_vma=False
    )
```

```python
import functools

import jax
import jax.numpy as jnp
from jax import lax
from jax.experimental import pallas as pl
from jax.experimental.pallas import tpu as pltpu
from jax.sharding import PartitionSpec as P

epsilon = 1e-06


def on_device(tokens, norm_gain, route, route_weight, gate_weight, up_weight, down_weight):
    tok_rows, width = tokens.shape
    top_count = route.shape[1]
    local_experts = gate_weight.shape[0]
    ep_count = lax.axis_size("ep")
    tp_count = lax.axis_size("tp")
    experts = local_experts * ep_count
    capacity = min(tok_rows, max(2, (3 * tok_rows * top_count + 2 * experts - 1) // (2 * experts)))
    width_share = width // tp_count
    values = tokens.astype(jnp.float32)
    scaled = values * lax.rsqrt(jnp.mean(values * values, axis=-1, keepdims=True) + epsilon)
    normed = (scaled * norm_gain).astype(jnp.bfloat16)
    flat_route = route.reshape(tok_rows * top_count)
    onehot = (flat_route[:, None] == jnp.arange(experts, dtype=jnp.int32)[None, :]).astype(
        jnp.int32
    )
    slot_number = jnp.sum((jnp.cumsum(onehot, axis=0) - 1) * onehot, axis=-1)
    slot_index = flat_route * capacity + slot_number
    placing = (
        slot_index[None, :] == jnp.arange(experts * capacity, dtype=jnp.int32)[:, None]
    ).astype(jnp.bfloat16)
    repeated = jnp.repeat(normed, top_count, axis=0)
    columns = lax.dynamic_slice_in_dim(repeated, lax.axis_index("tp") * width_share, width_share, 1)
    send = jnp.dot(placing, columns, preferred_element_type=jnp.float32).astype(jnp.bfloat16)
    send = send.reshape(ep_count, local_experts, capacity, width_share)
    arrived = lax.all_to_all(send, "ep", split_axis=0, concat_axis=0, tiled=True)
    piece = lax.all_gather(arrived, "tp", axis=3, tiled=True)
    gate = jnp.einsum("sjcd,jfd->sjcf", piece, gate_weight, preferred_element_type=jnp.float32)
    upward = jnp.einsum("sjcd,jfd->sjcf", piece, up_weight, preferred_element_type=jnp.float32)
    hidden = (jax.nn.silu(gate) * upward).astype(jnp.bfloat16)
    partial_value = jnp.einsum(
        "sjcf,jfd->sjcd", hidden, down_weight, preferred_element_type=jnp.float32
    )
    shares = lax.psum_scatter(
        partial_value.astype(jnp.bfloat16), "tp", scatter_dimension=3, tiled=True
    )
    returned = lax.all_to_all(shares, "ep", split_axis=0, concat_axis=0, tiled=True)
    results = returned.reshape(experts * capacity, width_share)
    picked = results[slot_index].reshape(tok_rows, top_count, width_share).astype(jnp.float32)
    mixed = jnp.sum(route_weight[:, :, None] * picked, axis=1)
    return mixed.astype(jnp.bfloat16)

MESH = pl.DeviceIdType.MESH
CORES = 2
F32 = jnp.float32
BF16 = jnp.bfloat16
NT = (((1,), (1,)), ((), ()))


def row_blocks(total, size):
    return [(at, min(size, total - at)) for at in range(0, total, size)]


def fused(
    nz, side, tokens_in, gain_in, route_in, weight_in, gate_hbm, up_hbm, down_hbm, out_ref,
    wg, wu, wd, xg, acc_g, acc_u, hid, ob, sib, ss, rp, zs, zr, wsend, wrecv,
    tokens_ref, gain_ref, route_ref, weight_ref, in_sem, w_sem, z_ssem, z_rsem, own_ssem, own_rsem, f_ssem, f_rsem, t_ssem, t_rsem,
    r_ssem, r_rsem, s_ssem, s_rsem, x_ssem, x_rsem, y_ssem, y_rsem,
):
    ep, tp = lax.axis_index("ep"), lax.axis_index("tp")
    n_tp, n_ep = side * side, nz * CORES
    z, core = ep // CORES, ep % CORES
    ty, tx = tp // side, tp % side
    rows, width = tokens_ref.shape
    small = [
        pltpu.make_async_copy(src, dst, in_sem.at[at])
        for at, (src, dst) in enumerate((
            (tokens_in, tokens_ref), (gain_in, gain_ref), (route_in, route_ref), (weight_in, weight_ref),
        ))
    ]
    for copy in small:
        copy.start()
    share = width // n_tp
    half = nz * rows

    def z_at(dz):
        at, bit = 0, 1
        while bit < nz:
            at = at + lax.rem(z // bit + dz // bit, 2) * bit
            bit = bit * 2
        return at

    from_z = z_at

    def quarter(r):
        return lax.rem(ty + r // side, side) * side + lax.rem(tx + r % side, side)

    def ep_id(zz, cc):
        return zz * CORES + cc

    other = 1 - core
    sibling = ep_id(z, other)

    def part(r):
        return pl.ds(r * share, share)

    def place(cc, zz):
        return pl.ds(pl.multiple_of((cc * nz + zz) * rows, rows), rows)

    barrier = pltpu.get_barrier_semaphore()
    for step in range(1, n_ep):
        pl.semaphore_signal(
            barrier, inc=1, device_id={"ep": lax.rem(ep + step, n_ep)}, device_id_type=MESH
        )
    for r in range(1, n_tp):
        pl.semaphore_signal(barrier, inc=1, device_id={"tp": quarter(r)}, device_id_type=MESH)

    loads = {}
    for r in range(n_tp):
        cols = pl.ds(pl.multiple_of(quarter(r) * share, share), share)
        for which, (hbm, vmem) in enumerate(((gate_hbm, wg), (up_hbm, wu), (down_hbm, wd))):
            loads[which, r] = pltpu.make_async_copy(
                hbm.at[0, :, cols], vmem.at[:, part(r)], w_sem.at[which, r]
            )
    for r in range(n_tp):
        loads[0, r].start()
        loads[1, r].start()
    for r in reversed(range(n_tp)):
        loads[2, r].start()

    for copy in small:
        copy.wait()
    values = tokens_ref[...].astype(F32)
    scaled = values * lax.rsqrt(jnp.mean(values * values, axis=-1, keepdims=True) + epsilon)
    normed = (scaled * gain_ref[...][None, :]).astype(BF16)
    for q in range(n_tp):
        qy, qx = q // side, q % side
        rel = lax.rem(qy + side - ty, side) * side + lax.rem(qx + side - tx, side)
        xg[rel, place(core, z), :] = normed[:, q * share : (q + 1) * share]
    position = (core * nz + z) * rows
    lanes = lax.broadcasted_iota(jnp.int32, (rows, n_ep * rows), 1)
    sublanes = lax.broadcasted_iota(jnp.int32, (rows, n_ep * rows), 0)
    spread = lanes == sublanes + position
    route, route_weight = route_ref[...], weight_ref[...]
    experts = lax.broadcasted_iota(jnp.int32, (n_ep, rows), 0)
    chosen = jnp.zeros((n_ep, rows), F32)
    for k in range(route.shape[0]):
        chosen = chosen + jnp.where(experts == route[k : k + 1], route_weight[k : k + 1], 0.0)
    chosen = chosen.T
    for e in range(n_ep):
        wsend[e] = jnp.sum(jnp.where(spread, chosen[:, e : e + 1], 0.0), axis=0, keepdims=True)
    pl.semaphore_wait(barrier, n_ep + n_tp - 2)

    def remote(src, dst, ssem, rsem, target):
        return pltpu.make_async_remote_copy(
            src_ref=src, dst_ref=dst, send_sem=ssem, recv_sem=rsem,
            device_id=target, device_id_type=MESH,
        )

    sent = []

    def go(copy):
        copy.start()
        sent.append(copy)
        return copy

    z_order = list(range(1, nz))
    z_copy = {}
    own = (0, place(core, z))
    for dz in z_order:
        z_copy[dz] = go(remote(
            xg.at[own], xg.at[own], z_ssem.at[dz], z_rsem.at[dz], {"ep": ep_id(z_at(dz), core)}
        ))
    across = (n_tp - 1, place(core, z))
    t_copy = {(n_tp - 1, 1): go(remote(
        xg.at[across], xg.at[across], t_ssem.at[n_tp - 1, 1], t_rsem.at[n_tp - 1, 1],
        {"ep": ep_id(z_at(1), core)},
    ))}
    own_copy = go(remote(
        xg.at[:, place(core, z)], xg.at[:, place(core, z)], own_ssem, own_rsem, {"ep": sibling}
    ))
    w_copy = []
    for step in range(1, n_ep):
        to = lax.rem(ep + step, n_ep)
        w_copy.append(go(remote(
            wsend.at[to], wrecv.at[step], r_ssem.at[step], r_rsem.at[step], {"ep": to}
        )))

    forward = {}
    for dz in z_order:
        z_copy[dz].wait_recv()
        block = (0, place(core, from_z(dz)))
        forward[0, dz] = go(remote(
            xg.at[block], xg.at[block], f_ssem.at[0, dz], f_rsem.at[0, dz], {"ep": sibling}
        ))
        for r in range(1, n_tp - 1):
            there = (r, place(core, from_z(dz)))
            t_copy[r, dz] = go(remote(
                xg.at[block], xg.at[there], t_ssem.at[r, dz], t_rsem.at[r, dz], {"tp": quarter(r)}
            ))
    for dz in z_order[1:]:
        r = n_tp - 1
        block, there = (0, place(core, from_z(dz))), (r, place(core, from_z(dz)))
        t_copy[r, dz] = go(remote(
            xg.at[block], xg.at[there], t_ssem.at[r, dz], t_rsem.at[r, dz], {"tp": quarter(r)}
        ))

    def pass_on(r):
        for dz in z_order:
            t_copy[r, dz].wait_recv()
            block = (r, place(core, from_z(dz)))
            forward[r, dz] = go(remote(
                xg.at[block], xg.at[block], f_ssem.at[r, dz], f_rsem.at[r, dz], {"ep": sibling}
            ))

    def forwarded(r):
        for dz in z_order:
            forward[r, dz].wait_recv()

    hidden_rows = wg.shape[0]
    blocks = row_blocks(hidden_rows, 5 * 128)
    own_copy.wait_recv()
    forwarded(0)

    def project(first, last):
        cols = slice(first * share, last * share)
        for r in range(first, last):
            loads[0, r].wait()
            loads[1, r].wait()
        held = jnp.concatenate([xg[r] for r in range(first, last)], axis=1)
        for at, size in blocks:
            for weights, acc in ((wg, acc_g), (wu, acc_u)):
                term = lax.dot_general(
                    weights[at : at + size, cols], held, NT, preferred_element_type=F32
                )
                acc[at : at + size, :] = term if first == 0 else acc[at : at + size, :] + term

    project(0, 1)
    for r in range(1, n_tp - 1):
        pass_on(r)
    for r in range(1, n_tp - 1):
        forwarded(r)
    project(1, n_tp - 1)
    pass_on(n_tp - 1)
    forwarded(n_tp - 1)
    for copy in w_copy:
        copy.wait_recv()
    mix = wsend[ep]
    for step in range(1, n_ep):
        mix = mix + wrecv[step]
    last = n_tp - 1
    loads[0, last].wait()
    loads[1, last].wait()
    cols = slice(last * share, n_tp * share)
    held = xg[last]
    for at, size in blocks:
        gate = acc_g[at : at + size, :] + lax.dot_general(
            wg[at : at + size, cols], held, NT, preferred_element_type=F32
        )
        upward = acc_u[at : at + size, :] + lax.dot_general(
            wu[at : at + size, cols], held, NT, preferred_element_type=F32
        )
        mixed_hidden = (gate / (1.0 + jnp.exp(-gate))) * upward * mix
        hid[:, at : at + size] = mixed_hidden.T.astype(BF16)

    mine = pl.ds(pl.multiple_of(core * half, half), half)
    yours = pl.ds(pl.multiple_of(other * half, half), half)
    back_order = list(reversed(range(n_tp)))
    far_order = list(reversed(z_order))
    s_copy, x_copy = {}, {}

    def combine(r):
        s_copy[r].wait_recv()
        total = ob[r, mine, :].astype(F32) + sib[r].astype(F32)
        ss[r] = total.astype(BF16)
        if r > 0:
            for dz in far_order + [0]:
                block = pl.ds(pl.multiple_of(z_at(dz) * rows, rows), rows)
                x_copy[r, dz] = go(remote(
                    ss.at[r, block, :], rp.at[r, block, :], x_ssem.at[r, dz], x_rsem.at[r, dz],
                    {"tp": quarter(r)},
                ))

    for k, r in enumerate(back_order):
        loads[2, r].wait()
        product = jnp.dot(hid[...], wd[:, r * share : (r + 1) * share], preferred_element_type=F32)
        ob[r] = product.astype(BF16)
        s_copy[r] = go(remote(
            ob.at[r, yours, :], sib.at[r], s_ssem.at[r], s_rsem.at[r], {"ep": sibling}
        ))
        if k > 0:
            combine(back_order[k - 1])
    combine(0)
    y_copy = {}
    for dz in far_order + [0]:
        block = pl.ds(pl.multiple_of(z_at(dz) * rows, rows), rows)
        total = ss[0, block, :].astype(F32)
        for r in range(1, n_tp):
            x_copy[r, dz].wait_recv()
            total = total + rp[r, block, :].astype(F32)
        if dz > 0:
            zs[dz] = total.astype(BF16)
            y_copy[dz] = go(remote(
                zs.at[dz], zr.at[dz], y_ssem.at[dz], y_rsem.at[dz], {"ep": ep_id(z_at(dz), core)}
            ))
    for dz in far_order:
        y_copy[dz].wait_recv()
        total = total + zr[dz].astype(F32)
    out_ref[...] = total.astype(BF16)
    for copy in sent:
        copy.wait_send()


def fused_call(nz, side, tokens, norm_gain, route, route_weight, gate_weight, up_weight, down_weight):
    rows, width = tokens.shape
    n_tp, n_ep = side * side, nz * CORES
    share, every, half = width // n_tp, n_ep * rows, nz * rows
    hidden = gate_weight.shape[1]
    vmem, dma = pltpu.VMEM, pltpu.SemaphoreType.DMA
    return pl.pallas_call(
        functools.partial(fused, nz, side),
        out_shape=jax.ShapeDtypeStruct((rows, share), BF16),
        in_specs=[pl.BlockSpec(memory_space=pl.ANY)] * 7,
        out_specs=pl.BlockSpec(memory_space=pltpu.VMEM),
        scratch_shapes=[
            vmem((hidden, width), BF16),
            vmem((hidden, width), BF16),
            vmem((hidden, width), BF16),
            vmem((n_tp, every, share), BF16),
            vmem((hidden, every), F32),
            vmem((hidden, every), F32),
            vmem((every, hidden), BF16),
            vmem((n_tp, every, share), BF16),
            vmem((n_tp, half, share), BF16),
            vmem((n_tp, half, share), BF16),
            vmem((n_tp, half, share), BF16),
            vmem((nz, rows, share), BF16),
            vmem((nz, rows, share), BF16),
            vmem((n_ep, 1, every), F32),
            vmem((n_ep, 1, every), F32),
            vmem(tokens.shape, BF16),
            vmem(norm_gain.shape, F32),
            vmem(route.T.shape, jnp.int32),
            vmem(route.T.shape, F32),
            dma((4,)),
            dma((3, n_tp)),
            dma((nz,)), dma((nz,)),
            dma, dma,
            dma((n_tp, nz)), dma((n_tp, nz)),
            dma((n_tp, nz)), dma((n_tp, nz)),
            dma((n_ep,)), dma((n_ep,)),
            dma((n_tp,)), dma((n_tp,)),
            dma((n_tp, nz)), dma((n_tp, nz)),
            dma((nz,)), dma((nz,)),
        ],
        compiler_params=pltpu.CompilerParams(
            collective_id=0, has_side_effects=True, vmem_limit_bytes=60 * 1024 * 1024
        ),
    )(tokens, norm_gain, route.T, route_weight.T, gate_weight, up_weight, down_weight)


def solution(mesh):
    n_ep, n_tp = mesh.shape["ep"], mesh.shape["tp"]
    side = 2

    def body(tokens, norm_gain, route, route_weight, gate_weight, up_weight, down_weight):
        args = (tokens, norm_gain, route, route_weight, gate_weight, up_weight, down_weight)
        fits = (
            n_tp == side * side
            and n_ep % CORES == 0
            and n_ep // CORES > 1
            and (n_ep // CORES) & (n_ep // CORES - 1) == 0
            and gate_weight.shape[0] == 1
            and tokens.shape[0] % 16 == 0
            and tokens.shape[1] % (128 * n_tp) == 0
            and gate_weight.shape[1] % 16 == 0
        )
        if fits:
            return fused_call(n_ep // CORES, side, *args)
        return on_device(*args)

    placed = (
        P("ep", None),
        P(),
        P("ep", None),
        P("ep", None),
        P("ep", "tp", None),
        P("ep", "tp", None),
        P("ep", "tp", None),
    )
    return jax.shard_map(
        body, mesh=mesh, in_specs=placed, out_specs=P("ep", "tp"), check_vma=False
    )
```
